32 devices in a mesh: sp: 8 (over z, y), tp: 4 (over x, core).
Axes of the slice: x: 2, y: 2, z: 4, core: 2. Of those that a mesh axis runs over, the one named last changes fastest.
Arguments:
- mixer_input: bfloat16 [2048, 2048], P('sp', 'tp'), may hold values from -6 to 6
- step_log: float32 [2048, 128], P('sp'), may hold values from -4.21 to -1.89
- forget_log: float32 [2048, 128], P('sp'), may hold values from -0.7 to 0
- decay_rate: float32 [128, 64], replicated, may hold values from 0 to 0.8
- frequency: float32 [128, 64], replicated, may hold values from 1 to 64
- input_map: float32 [2, 128, 64, 16], P(None, 'tp'), may hold values from -2.5 to 2.5
- output_map: float32 [2, 128, 16, 64], P(None, 'tp'), may hold values from -1.25 to 1.25
- skip_gain: float32 [2048], replicated, may hold values from -3 to 3
- value_weight: bfloat16 [2048, 2048], replicated, may hold values from -0.125 to 0.125
- gate_weight: bfloat16 [2048, 2048], replicated, may hold values from -0.125 to 0.125
- residual: bfloat16 [2048, 2048], P(('sp', 'tp')), may hold values from -6 to 6
- norm_gain: bfloat16 [2048], replicated, may hold values from 0.099609375 to 1.8984375
- ffn_gate: bfloat16 [2048, 5632], P('sp', 'tp'), may hold values from -0.125 to 0.125
- ffn_up: bfloat16 [2048, 5632], P('sp', 'tp'), may hold values from -0.125 to 0.125
- conv_taps: float32 [3, 5632], replicated, may hold values from -6 to 6
- ffn_down: bfloat16 [5632, 2048], P('tp', 'sp'), may hold values from -0.078125 to 0.078125
Outputs:
- updated: bfloat16 [2048, 2048], P(('sp', 'tp'))
The draws below stay inside these ranges and needn't reach their ends.
All inputs are finite; a program needn't handle non-finite values.
Results may differ from the reference program's by a relative error of at most 0.014.
Values may be sent and summed in bfloat16 or wider, within the bound.
A program may use at most 192 MiB of HBM per device.

```python
import math
import jax
import jax.numpy as jnp
from jax import lax

D = 2048
CHANNELS = 16
GROUPS = 128
STATE = 64
FF = 5632
CONV = 3
TOK_DEV = 256
TOKENS = 2048
N_TP = 4


def draw_step_log(key, part):
    block_key, jitter_key = jax.random.split(jax.random.fold_in(key, 11), 2)
    blocks = TOKENS // TOK_DEV
    block_factor = jax.random.uniform(block_key, (blocks, 1, GROUPS), jnp.float32, math.log(0.5), math.log(2.0))
    jitter = jax.random.uniform(jitter_key, (blocks, TOK_DEV, GROUPS), jnp.float32, math.log(0.6), math.log(1.5))
    return (math.log(0.05) + block_factor + jitter).reshape(TOKENS, GROUPS)


def draw_forget_log(key, part):
    place_key, loss_key = jax.random.split(jax.random.fold_in(key, 37), 2)
    places = jax.random.randint(place_key, (6,), 0, 3 * TOKENS // 4)
    hit = jnp.any(jnp.arange(TOKENS)[:, None] == places[None, :], axis=1)
    losses = jnp.log(jax.random.uniform(loss_key, (TOKENS, GROUPS), jnp.float32, 0.5, 0.8))
    return jnp.where(hit[:, None], losses, jnp.zeros((TOKENS, GROUPS), jnp.float32))


def draw_decay_rate(key, part):
    class_key, slow_key, fast_key = jax.random.split(jax.random.fold_in(key, 23), 3)
    slow_share = 0.5
    slow = jax.random.bernoulli(class_key, slow_share, (GROUPS, 1))
    slow_rate = jax.random.uniform(slow_key, (GROUPS, STATE), jnp.float32, 0.25, 0.55) / (0.05 * TOKENS)
    fast_rate = jnp.exp(jax.random.uniform(fast_key, (GROUPS, STATE), jnp.float32, math.log(0.3), math.log(0.8)))
    return jnp.where(slow, slow_rate, fast_rate)


def block_levels(rng, extent, cuts, least, top_value):
    level = 1.0
    for axis_at, parts in cuts:
        heights = jax.random.uniform(jax.random.fold_in(jax.random.fold_in(rng, 6), axis_at), (parts,), jnp.float32, least / len(cuts), top_value / len(cuts))
        level = level * jnp.repeat(jnp.exp(heights), extent[axis_at] // parts).reshape((-1,) + (1,) * (len(extent) - 1 - axis_at))
    return level


def normal_values(rng, shape, deviation, limit, pieces=(), held_as=jnp.bfloat16):
    drawn = deviation * jax.random.normal(rng, shape, jnp.float32)
    if pieces:
        drawn = drawn * block_levels(rng, shape, pieces, -0.22, 0.18)
    return jnp.clip(drawn, -limit, limit).astype(held_as)


def setup_inputs(seed: int = 0) -> dict:
    key_list = jax.random.split(jax.random.key(seed), 17)
    mixer_input = normal_values(key_list[0], (TOKENS, D), 1.0, 6.0, ((0, 8), (1, 4)))
    step_log = draw_step_log(jax.random.fold_in(key_list[16], 71), 0)
    forget_log = draw_forget_log(jax.random.fold_in(key_list[16], 71), 0)
    decay_rate = draw_decay_rate(jax.random.fold_in(key_list[16], 71), 0)
    frequency = jnp.clip(jax.random.uniform(key_list[4], (GROUPS, STATE), jnp.float32, 1.0, 64.0), 1.0, 64.0)
    input_map = normal_values(key_list[5], (2, GROUPS, STATE, CHANNELS), ((2 * CHANNELS) ** -0.5), 2.5, ((1, 4),), jnp.float32)
    output_map = normal_values(key_list[6], (2, GROUPS, CHANNELS, STATE), ((2 * STATE) ** -0.5), 1.25, ((1, 4),), jnp.float32)
    skip_gain = normal_values(key_list[7], (D,), 0.5, 3.0, (), jnp.float32)
    value_weight = normal_values(key_list[8], (D, D), D ** -0.5, 0.125)
    gate_weight = normal_values(key_list[9], (D, D), D ** -0.5, 0.125)
    residual = normal_values(key_list[10], (TOKENS, D), 1.0, 6.0, ((0, 32),))
    norm_gain = jnp.clip(1.0 + 0.18 * jax.random.normal(key_list[11], (D,), jnp.float32), 0.099609375, 1.8984375).astype(jnp.bfloat16)
    ffn_gate = normal_values(key_list[12], (D, FF), D ** -0.5, 0.125, ((0, 8), (1, 4)))
    ffn_up = normal_values(key_list[13], (D, FF), D ** -0.5, 0.125, ((0, 8), (1, 4)))
    conv_taps = normal_values(key_list[14], (CONV, FF), (CONV ** -0.5), 6.0, (), jnp.float32)
    ffn_down = normal_values(key_list[15], (FF, D), FF ** -0.5, 0.078125, ((0, 4), (1, 8)))
    return {"mixer_input": mixer_input, "step_log": step_log, "forget_log": forget_log, "decay_rate": decay_rate, "frequency": frequency, "input_map": input_map, "output_map": output_map, "skip_gain": skip_gain, "value_weight": value_weight, "gate_weight": gate_weight, "residual": residual, "norm_gain": norm_gain, "ffn_gate": ffn_gate, "ffn_up": ffn_up, "conv_taps": conv_taps, "ffn_down": ffn_down}


def compose(earlier, later):
    decay_real = later[0] * earlier[0] - later[1] * earlier[1]
    decay_imag = later[0] * earlier[1] + later[1] * earlier[0]
    state_real = later[0] * earlier[2] - later[1] * earlier[3] + later[2]
    state_imag = later[0] * earlier[3] + later[1] * earlier[2] + later[3]
    return (decay_real, decay_imag, state_real, state_imag)

def reference(mixer_input, step_log, forget_log, decay_rate, frequency, input_map, output_map, skip_gain, value_weight, gate_weight, residual, norm_gain, ffn_gate, ffn_up, conv_taps, ffn_down):
    blocks = TOKENS // TOK_DEV
    flat = GROUPS * STATE
    real_part = -decay_rate[None]
    omega = frequency[None]
    divisor = real_part * real_part + omega * omega
    portion = FF // N_TP
    history = CONV - 1
    gain = norm_gain.astype(jnp.float32)

    def advance(carry, inputs):
        carry_real, carry_imag, gate_tail = carry
        signal_half, log_step, log_forget, residual_rows = inputs
        steps = jnp.exp(log_step)[:, :, None]
        magnitude = jnp.exp(real_part * steps)
        angle = omega * steps
        held_real = magnitude * jnp.cos(angle)
        held_imag = magnitude * jnp.sin(angle)
        factor_real = ((held_real - 1.0) * real_part + held_imag * omega) / divisor
        factor_imag = (held_imag * real_part - (held_real - 1.0) * omega) / divisor
        retained = jnp.exp(log_forget)[:, :, None]
        decay_real = (retained * held_real).reshape(TOK_DEV, flat)
        decay_imag = (retained * held_imag).reshape(TOK_DEV, flat)
        signal = signal_half.astype(jnp.float32)
        grouped = signal.reshape(TOK_DEV, GROUPS, CHANNELS)
        mapped_real = jnp.einsum('tgh,gph->tgp', grouped, input_map[0], precision=lax.Precision.HIGHEST)
        mapped_imag = jnp.einsum('tgh,gph->tgp', grouped, input_map[1], precision=lax.Precision.HIGHEST)
        drive_real = (factor_real * mapped_real - factor_imag * mapped_imag).reshape(TOK_DEV, flat)
        drive_imag = (factor_real * mapped_imag + factor_imag * mapped_real).reshape(TOK_DEV, flat)
        prefix = lax.associative_scan(compose, (decay_real, decay_imag, drive_real, drive_imag), axis=0)
        state_real = prefix[2] + prefix[0] * carry_real - prefix[1] * carry_imag
        state_imag = prefix[3] + prefix[0] * carry_imag + prefix[1] * carry_real
        response = (jnp.einsum('tgp,ghp->tgh', state_real.reshape(TOK_DEV, GROUPS, STATE), output_map[0], precision=lax.Precision.HIGHEST) - jnp.einsum('tgp,ghp->tgh', state_imag.reshape(TOK_DEV, GROUPS, STATE), output_map[1], precision=lax.Precision.HIGHEST)).reshape(TOK_DEV, D)
        response = response + skip_gain * signal
        activated = jax.nn.gelu(response).astype(jnp.bfloat16)
        value = jnp.dot(activated, value_weight, preferred_element_type=jnp.float32)
        gate = jnp.dot(activated, gate_weight, preferred_element_type=jnp.float32)
        mixed = value * jax.nn.sigmoid(gate)
        stream = (residual_rows.astype(jnp.float32) + mixed).astype(jnp.bfloat16)
        stream_wide = stream.astype(jnp.float32)
        scale = lax.rsqrt(lax.optimization_barrier(jnp.mean(stream_wide * stream_wide, axis=1, keepdims=True)) + 1e-06)
        normed = (stream_wide * scale * gain).astype(jnp.bfloat16)
        gate_pre = jnp.dot(normed, ffn_gate, preferred_element_type=jnp.float32)
        up_pre = jnp.dot(normed, ffn_up, preferred_element_type=jnp.float32)
        extended = jnp.concatenate([gate_tail, gate_pre], axis=0)
        conv_gate = conv_taps[0] * extended[0:TOK_DEV]
        for offset in range(1, CONV):
            conv_gate = conv_gate + conv_taps[offset] * extended[offset:offset + TOK_DEV]
        hidden = (jax.nn.silu(conv_gate) * up_pre).astype(jnp.bfloat16)
        ffn_out = jnp.zeros((TOK_DEV, D), jnp.float32)
        for index in range(N_TP):
            lower = index * portion
            partial_value = jnp.dot(hidden[:, lower:lower + portion], ffn_down[lower:lower + portion], preferred_element_type=jnp.float32)
            ffn_out = ffn_out + lax.optimization_barrier(partial_value.astype(jnp.bfloat16)).astype(jnp.float32)
        updated = (stream_wide + ffn_out).astype(jnp.bfloat16)
        return ((state_real[-1], state_imag[-1], gate_pre[TOK_DEV - history:]), updated)
    start = (jnp.zeros((flat,), jnp.float32), jnp.zeros((flat,), jnp.float32), jnp.zeros((history, FF), jnp.float32))
    inputs = (mixer_input.reshape(blocks, TOK_DEV, D), step_log.reshape(blocks, TOK_DEV, GROUPS), forget_log.reshape(blocks, TOK_DEV, GROUPS), residual.reshape(blocks, TOK_DEV, D))
    final, outputs = lax.scan(advance, start, inputs)
    return outputs.reshape(TOKENS, D)
```

```python
import functools
import math

import jax
import jax.numpy as jnp
from jax import lax
from jax.experimental import pallas as pl
from jax.experimental.pallas import tpu as pltpu
from jax.sharding import PartitionSpec as P

LANES = 128
SEGMENTS = 8
CHUNK = 64


def sin_cos(angle):
    turns = jnp.floor(angle * (1.0 / math.pi) + 0.5)
    r = angle - turns * 3.140625
    r = r - turns * 9.67025756835937500e-4
    r = r - turns * 6.278329571113e-7
    half = turns * 0.5
    sign = 1.0 - 4.0 * (half - jnp.floor(half))
    q = r * r
    s = -2.3889859e-08
    for c in (2.7525562e-06, -1.9840874e-04, 8.3333310e-03, -1.6666667e-01):
        s = s * q + c
    s = r + r * (q * s)
    c_ = 2.0875723e-09
    for c in (-2.7557314e-07, 2.4801587e-05, -1.3888889e-03, 4.1666667e-02, -0.5):
        c_ = c_ * q + c
    c_ = 1.0 + q * c_
    return sign * s, sign * c_


def ssm_kernel(
    n_sp, groups, per_tile, tiles_per_block,
    x_ref, step_ref, forget_ref, rate_ref, w_in_ref, w_out_ref, skip_ref, out_ref,
    steps, kept, pr, pi, sr, si, fin, excl, summary, slots, before, packed, resp,
    send_sem, recv_sem,
):
    me = lax.axis_index("sp")
    first = lax.axis_index("tp") * groups
    rows = x_ref.shape[0]
    tiles = w_in_ref.shape[0]
    span = rows // SEGMENTS
    width = step_ref.shape[1]
    entries = LANES // per_tile

    if n_sp > 1:
        barrier = pltpu.get_barrier_semaphore()
        for d in range(1, n_sp):
            pl.semaphore_signal(
                barrier, inc=1, device_id={"sp": lax.rem(me + d, n_sp)},
                device_id_type=pl.DeviceIdType.MESH,
            )

    steps[...] = jnp.exp(step_ref[...])
    kept[...] = jnp.exp(forget_ref[...])

    def spread(array, shape):
        lane = lax.broadcasted_iota(jnp.int32, shape, 1)
        result = jnp.broadcast_to(array[:, 0:1], shape)
        for j in range(1, per_tile):
            result = jnp.where(lane < j * entries, result, array[:, j : j + 1])
        return result

    def tile(k, carry):
        block = pl.multiple_of((k // tiles_per_block) * LANES, LANES)
        shift = lax.rem(2 * width - (first + per_tile * k), width)
        a_real = rate_ref[0, pl.ds(k, 1), :]
        omega = rate_ref[1, pl.ds(k, 1), :]
        c_real = rate_ref[2, pl.ds(k, 1), :]
        c_imag = rate_ref[3, pl.ds(k, 1), :]
        for start in range(0, rows, CHUNK):
            at = pl.ds(start, CHUNK)
            shape = (CHUNK, LANES)
            step = spread(pltpu.roll(steps[at, :], shift, 1), shape)
            keep = spread(pltpu.roll(kept[at, :], shift, 1), shape)
            magnitude = jnp.exp(a_real * step)
            sine, cosine = sin_cos(omega * step)
            held_real = magnitude * cosine
            held_imag = magnitude * sine
            pr[k, at, :] = keep * held_real
            pi[k, at, :] = keep * held_imag
            less = held_real - 1.0
            factor_real = less * c_real + held_imag * c_imag
            factor_imag = held_imag * c_real - less * c_imag
            mapped = jnp.dot(
                x_ref[at, pl.ds(block, LANES)], w_in_ref[k],
                preferred_element_type=jnp.float32,
            )
            m_real, m_imag = mapped[:, :LANES], mapped[:, LANES:]
            sr[k, at, :] = factor_real * m_real - factor_imag * m_imag
            si[k, at, :] = factor_real * m_imag + factor_imag * m_real
        at = pl.ds(0, SEGMENTS, stride=span)
        p_r, p_i = pr[k, at, :], pi[k, at, :]
        s_r, s_i = sr[k, at, :], si[k, at, :]
        for j in range(1, span):
            at = pl.ds(j, SEGMENTS, stride=span)
            a_r, a_i = pr[k, at, :], pi[k, at, :]
            s_r, s_i = (
                a_r * s_r - a_i * s_i + sr[k, at, :],
                a_r * s_i + a_i * s_r + si[k, at, :],
            )
            p_r, p_i = a_r * p_r - a_i * p_i, a_r * p_i + a_i * p_r
            pr[k, at, :] = p_r
            pi[k, at, :] = p_i
            sr[k, at, :] = s_r
            si[k, at, :] = s_i
        for c, value in enumerate((p_r, p_i, s_r, s_i)):
            fin[c] = value
        t_r = jnp.ones((1, LANES), jnp.float32)
        t_i = jnp.zeros((1, LANES), jnp.float32)
        u_r, u_i = t_i, t_i
        for s in range(SEGMENTS):
            for c, value in enumerate((t_r, t_i, u_r, u_i)):
                excl[c, k, pl.ds(s, 1), :] = value
            a_r, a_i = fin[0, pl.ds(s, 1), :], fin[1, pl.ds(s, 1), :]
            b_r, b_i = fin[2, pl.ds(s, 1), :], fin[3, pl.ds(s, 1), :]
            t_r, t_i = a_r * t_r - a_i * t_i, a_r * t_i + a_i * t_r
            u_r, u_i = a_r * u_r - a_i * u_i + b_r, a_r * u_i + a_i * u_r + b_i
        for c, value in enumerate((t_r, t_i, u_r, u_i)):
            summary[c, pl.ds(k, 1), :] = value
        return carry

    lax.fori_loop(0, tiles, tile, 0)

    def copy(d):
        return pltpu.make_async_remote_copy(
            src_ref=summary, dst_ref=slots.at[d - 1],
            send_sem=send_sem.at[d - 1], recv_sem=recv_sem.at[d - 1],
            device_id={"sp": lax.rem(me + d, n_sp)},
            device_id_type=pl.DeviceIdType.MESH,
        )

    before[...] = jnp.zeros_like(before)
    if n_sp > 1:
        pl.semaphore_wait(barrier, n_sp - 1)
        for d in range(1, n_sp):
            @pl.when(me + d < n_sp)
            def _():
                copy(d).start()

    for start in range(0, resp.shape[1], LANES):
        at = pl.ds(start, LANES)
        resp[:, at] = skip_ref[:, at] * x_ref[:, at].astype(jnp.float32)

    for d in range(n_sp - 1, 0, -1):
        @pl.when(me >= d)
        def _():
            copy(d).wait_recv()
            a_r, a_i = slots[d - 1, 0], slots[d - 1, 1]
            h_r, h_i = before[0], before[1]
            before[0] = a_r * h_r - a_i * h_i + slots[d - 1, 2]
            before[1] = a_r * h_i + a_i * h_r + slots[d - 1, 3]

    def finish(k, carry):
        block = pl.multiple_of((k // tiles_per_block) * LANES, LANES)
        h_r, h_i = before[0, pl.ds(k, 1), :], before[1, pl.ds(k, 1), :]
        t_r, t_i = excl[0, k], excl[1, k]
        o_r = t_r * h_r - t_i * h_i + excl[2, k]
        o_i = t_r * h_i + t_i * h_r + excl[3, k]
        for s in range(SEGMENTS):
            at = pl.ds(s * span, span)
            b_r, b_i = o_r[s : s + 1, :], o_i[s : s + 1, :]
            a_r, a_i = pr[k, at, :], pi[k, at, :]
            packed[at, :LANES] = (sr[k, at, :] + a_r * b_r - a_i * b_i).astype(jnp.bfloat16)
            packed[at, LANES:] = (si[k, at, :] + a_r * b_i + a_i * b_r).astype(jnp.bfloat16)
        resp[:, pl.ds(block, LANES)] += jnp.dot(
            packed[...], w_out_ref[k], preferred_element_type=jnp.float32
        )
        return carry

    lax.fori_loop(0, tiles, finish, 0)
    for start in range(0, resp.shape[1], LANES):
        at = pl.ds(start, LANES)
        out_ref[:, at] = jax.nn.gelu(resp[:, at]).astype(out_ref.dtype)
    for d in range(1, n_sp):
        @pl.when(me + d < n_sp)
        def _():
            copy(d).wait_send()


def state_space(n_sp, x, step_log, forget_log, rate, freq, in_map, out_map, skip):
    rows, local_width = x.shape
    _, groups, entries, channels = in_map.shape
    per_tile = LANES // entries
    tiles = groups // per_tile
    per_block = LANES // channels
    tiles_per_block = per_block // per_tile
    a_real = -rate.reshape(tiles, LANES)
    omega = freq.reshape(tiles, LANES)
    divisor = a_real * a_real + omega * omega
    rates = jnp.stack([a_real, omega, a_real / divisor, omega / divisor])
    slot = jnp.arange(per_block)[None, :, None]
    own = per_tile * (jnp.arange(tiles) % tiles_per_block)
    mask = slot == own[:, None, None] + jnp.arange(per_tile)[None, None, :]
    w_in = in_map.astype(jnp.bfloat16).reshape(2, tiles, per_tile, entries, channels).transpose(1, 4, 0, 2, 3)
    w_in = jnp.where(mask[:, :, None, None, :, None], w_in[:, None], 0).reshape(tiles, LANES, 2 * LANES)
    sign = jnp.array([1.0, -1.0], jnp.float32)[:, None, None, None]
    w_out = (out_map * sign).astype(jnp.bfloat16).reshape(2, tiles, per_tile, channels, entries)
    w_out = w_out.transpose(1, 0, 2, 4, 3)[:, :, :, :, None, :]
    w_out = jnp.where(mask.transpose(0, 2, 1)[:, None, :, None, :, None], w_out, 0)
    w_out = w_out.reshape(tiles, 2 * LANES, LANES)
    vmem = pl.BlockSpec(memory_space=pltpu.VMEM)
    f32 = jnp.float32
    peers = max(n_sp - 1, 1)
    big = pltpu.VMEM((tiles, rows, LANES), f32)
    return pl.pallas_call(
        functools.partial(ssm_kernel, n_sp, groups, per_tile, tiles_per_block),
        out_shape=jax.ShapeDtypeStruct((rows, local_width), jnp.bfloat16),
        in_specs=[vmem] * 7,
        out_specs=vmem,
        scratch_shapes=[
            pltpu.VMEM(step_log.shape, f32), pltpu.VMEM(step_log.shape, f32),
            big, big, big, big,
            pltpu.VMEM((4, SEGMENTS, LANES), f32),
            pltpu.VMEM((4, tiles, SEGMENTS, LANES), f32),
            pltpu.VMEM((4, tiles, LANES), f32),
            pltpu.VMEM((peers, 4, tiles, LANES), f32),
            pltpu.VMEM((2, tiles, LANES), f32),
            pltpu.VMEM((rows, 2 * LANES), jnp.bfloat16),
            pltpu.VMEM((rows, local_width), f32),
            pltpu.SemaphoreType.DMA((peers,)),
            pltpu.SemaphoreType.DMA((peers,)),
        ],
        compiler_params=pltpu.CompilerParams(
            collective_id=0, has_side_effects=True, vmem_limit_bytes=40 * 2**20,
        ),
        cost_estimate=pl.CostEstimate(
            flops=60_000_000_000, bytes_accessed=4_000_000, transcendentals=0
        ),
    )(x, step_log, forget_log, rates, w_in, w_out, skip)


def ring_tables(n):
    if n % 2:
        return list(range(n))
    return list(range(0, n, 2)) + list(range(n - 1, 0, -2))


def ring_owner(n, position):
    if n % 2:
        return position
    return jnp.where(position < n // 2, 2 * position, 2 * (n - 1 - position) + 1)


def ring_position(n, index):
    if n % 2:
        return index
    return jnp.where(index % 2 == 0, index // 2, n - 1 - index // 2)


def ring_steps(n, block, direction):
    order = ring_tables(n)
    route = [(order[i], order[(i + direction) % n]) for i in range(n)]
    place = ring_position(n, lax.axis_index("sp"))
    for step in range(n):
        owner = ring_owner(n, lax.rem(place - direction * step + n * n, n))
        yield block, owner
        if step < n - 1:
            block = lax.ppermute(block, "sp", route)


def shifted_2(block, axis, distance):
    devices = range(lax.axis_size(axis))
    route = [(i - distance, i) for i in devices if i - distance in devices]
    return lax.ppermute(block, axis, route)


def local(
    mixer_input, step_log, forget_log, decay_rate, frequency, input_map, output_map,
    skip_gain, value_weight, gate_weight, residual, norm_gain, ffn_gate, ffn_up,
    conv_taps, ffn_down,
):
    tp_index = lax.axis_index("tp")
    n_sp = lax.axis_size("sp")
    tp_count = lax.axis_size("tp")
    positions, local_width = mixer_input.shape
    groups = input_map.shape[1]
    model = ffn_gate.shape[0] * n_sp
    hidden_width = ffn_gate.shape[1]

    gate_full = jnp.zeros((model, hidden_width), ffn_gate.dtype)
    up_full = jnp.zeros((model, hidden_width), ffn_up.dtype)
    depth = ffn_gate.shape[0]
    for block, owner in ring_steps(n_sp, ffn_gate, 1):
        gate_full = lax.dynamic_update_slice(gate_full, block, (owner * depth, 0))
        last_gate = block
    for block, owner in ring_steps(n_sp, ffn_up, -1):
        up_full = lax.dynamic_update_slice(up_full, block, (owner * depth, 0))
        last_up = block
    half = hidden_width // 2
    top, bottom = ffn_down[:half], ffn_down[half:]
    top, bottom, last_gate, last_up = lax.optimization_barrier((top, bottom, last_gate, last_up))
    down_full = jnp.zeros((hidden_width, model), ffn_down.dtype)
    wide = ffn_down.shape[1]
    for block, owner in ring_steps(n_sp, top, 1):
        down_full = lax.dynamic_update_slice(down_full, block, (0, owner * wide))
    for block, owner in ring_steps(n_sp, bottom, -1):
        down_full = lax.dynamic_update_slice(down_full, block, (half, owner * wide))

    activated = state_space(
        n_sp, mixer_input, step_log, forget_log,
        lax.dynamic_slice_in_dim(decay_rate, tp_index * groups, groups, 0),
        lax.dynamic_slice_in_dim(frequency, tp_index * groups, groups, 0),
        input_map, output_map,
        lax.dynamic_slice_in_dim(skip_gain, tp_index * local_width, local_width, 0)[None],
    )
    own_rows = positions // tp_count
    row_block = lax.all_to_all(
        activated.reshape(tp_count, own_rows, local_width),
        "tp", split_axis=0, concat_axis=2, tiled=True,
    )[0]
    value = jnp.dot(row_block, value_weight, preferred_element_type=jnp.float32)
    gate = jnp.dot(row_block, gate_weight, preferred_element_type=jnp.float32)
    mixed = value * jax.nn.sigmoid(gate)
    stream = (residual.astype(jnp.float32) + mixed).astype(jnp.bfloat16)
    stream_wide = stream.astype(jnp.float32)
    scale = lax.rsqrt(jnp.mean(stream_wide * stream_wide, axis=1, keepdims=True) + 1e-06)
    normed = (stream_wide * scale * norm_gain.astype(jnp.float32)).astype(jnp.bfloat16)
    whole_rows = lax.all_gather(normed, "tp", axis=0, tiled=True)
    gate_pre = jnp.dot(whole_rows, gate_full, preferred_element_type=jnp.float32)
    up_pre = jnp.dot(whole_rows, up_full, preferred_element_type=jnp.float32)
    history = conv_taps.shape[0] - 1
    boundary = shifted_2(gate_pre[positions - history :], "sp", 1)
    extended = jnp.concatenate([boundary, gate_pre], axis=0)
    tap_weights = lax.dynamic_slice_in_dim(conv_taps, tp_index * hidden_width, hidden_width, 1)
    conv_gate = tap_weights[0] * extended[0:positions]
    for offset in range(1, history + 1):
        conv_gate = conv_gate + tap_weights[offset] * extended[offset : offset + positions]
    hidden = (jax.nn.silu(conv_gate) * up_pre).astype(jnp.bfloat16)
    partial_value = jnp.dot(hidden, down_full, preferred_element_type=jnp.float32)
    ffn_out = lax.psum_scatter(
        partial_value.astype(jnp.bfloat16), "tp", scatter_dimension=0, tiled=True
    ).astype(jnp.float32)
    return (stream_wide + ffn_out).astype(jnp.bfloat16)


def solution(mesh):
    in_specs = (
        P("sp", "tp"), P("sp", None), P("sp", None), P(), P(),
        P(None, "tp", None, None), P(None, "tp", None, None),
        P(), P(), P(), P(("sp", "tp"), None), P(),
        P("sp", "tp"), P("sp", "tp"), P(), P("tp", "sp"),
    )
    out_specs = P(("sp", "tp"), None)
    return jax.shard_map(local, mesh=mesh, in_specs=in_specs, out_specs=out_specs, check_vma=False)
```

```python
import functools
import math

import jax
import jax.numpy as jnp
from jax import lax
from jax.experimental import pallas as pl
from jax.experimental.pallas import tpu as pltpu
from jax.sharding import PartitionSpec as P


LANES = 128
SEGMENTS = 8
CHUNK = 64


def sin_cos(angle):
    turns = jnp.floor(angle * (1.0 / math.pi) + 0.5)
    r = angle - turns * 3.140625
    r = r - turns * 9.67025756835937500e-4
    r = r - turns * 6.278329571113e-7
    half = turns * 0.5
    sign = 1.0 - 4.0 * (half - jnp.floor(half))
    q = r * r
    s = -2.3889859e-08
    for c in (2.7525562e-06, -1.9840874e-04, 8.3333310e-03, -1.6666667e-01):
        s = s * q + c
    s = r + r * (q * s)
    c_ = 2.0875723e-09
    for c in (-2.7557314e-07, 2.4801587e-05, -1.3888889e-03, 4.1666667e-02, -0.5):
        c_ = c_ * q + c
    c_ = 1.0 + q * c_
    return sign * s, sign * c_


def ssm_kernel(
    n_sp, groups, per_tile, tiles_per_block,
    x_ref, step_ref, forget_ref, rate_ref, w_in_ref, w_out_ref, skip_ref, out_ref,
    steps, kept, pr, pi, sr, si, fin, excl, summary, slots, before, packed, resp,
    send_sem, recv_sem,
):
    me = lax.axis_index("sp")
    first = lax.axis_index("tp") * groups
    rows = x_ref.shape[0]
    tiles = w_in_ref.shape[0]
    span = rows // SEGMENTS
    width = step_ref.shape[1]
    entries = LANES // per_tile

    if n_sp > 1:
        barrier = pltpu.get_barrier_semaphore()
        for d in range(1, n_sp):
            pl.semaphore_signal(
                barrier, inc=1, device_id={"sp": lax.rem(me + d, n_sp)},
                device_id_type=pl.DeviceIdType.MESH,
            )

    steps[...] = jnp.exp(step_ref[...])
    kept[...] = jnp.exp(forget_ref[...])

    def spread(array, shape):
        lane = lax.broadcasted_iota(jnp.int32, shape, 1)
        result = jnp.broadcast_to(array[:, 0:1], shape)
        for j in range(1, per_tile):
            result = jnp.where(lane < j * entries, result, array[:, j : j + 1])
        return result

    def tile(k, carry):
        block = pl.multiple_of((k // tiles_per_block) * LANES, LANES)
        shift = lax.rem(2 * width - (first + per_tile * k), width)
        a_real = rate_ref[0, pl.ds(k, 1), :]
        omega = rate_ref[1, pl.ds(k, 1), :]
        c_real = rate_ref[2, pl.ds(k, 1), :]
        c_imag = rate_ref[3, pl.ds(k, 1), :]
        for start in range(0, rows, CHUNK):
            at = pl.ds(start, CHUNK)
            shape = (CHUNK, LANES)
            step = spread(pltpu.roll(steps[at, :], shift, 1), shape)
            keep = spread(pltpu.roll(kept[at, :], shift, 1), shape)
            magnitude = jnp.exp(a_real * step)
            sine, cosine = sin_cos(omega * step)
            held_real = magnitude * cosine
            held_imag = magnitude * sine
            pr[k, at, :] = keep * held_real
            pi[k, at, :] = keep * held_imag
            less = held_real - 1.0
            factor_real = less * c_real + held_imag * c_imag
            factor_imag = held_imag * c_real - less * c_imag
            mapped = jnp.dot(
                x_ref[at, pl.ds(block, LANES)], w_in_ref[k],
                preferred_element_type=jnp.float32,
            )
            m_real, m_imag = mapped[:, :LANES], mapped[:, LANES:]
            sr[k, at, :] = factor_real * m_real - factor_imag * m_imag
            si[k, at, :] = factor_real * m_imag + factor_imag * m_real
        at = pl.ds(0, SEGMENTS, stride=span)
        p_r, p_i = pr[k, at, :], pi[k, at, :]
        s_r, s_i = sr[k, at, :], si[k, at, :]
        for j in range(1, span):
            at = pl.ds(j, SEGMENTS, stride=span)
            a_r, a_i = pr[k, at, :], pi[k, at, :]
            s_r, s_i = (
                a_r * s_r - a_i * s_i + sr[k, at, :],
                a_r * s_i + a_i * s_r + si[k, at, :],
            )
            p_r, p_i = a_r * p_r - a_i * p_i, a_r * p_i + a_i * p_r
            pr[k, at, :] = p_r
            pi[k, at, :] = p_i
            sr[k, at, :] = s_r
            si[k, at, :] = s_i
        for c, value in enumerate((p_r, p_i, s_r, s_i)):
            fin[c] = value
        t_r = jnp.ones((1, LANES), jnp.float32)
        t_i = jnp.zeros((1, LANES), jnp.float32)
        u_r, u_i = t_i, t_i
        for s in range(SEGMENTS):
            for c, value in enumerate((t_r, t_i, u_r, u_i)):
                excl[c, k, pl.ds(s, 1), :] = value
            a_r, a_i = fin[0, pl.ds(s, 1), :], fin[1, pl.ds(s, 1), :]
            b_r, b_i = fin[2, pl.ds(s, 1), :], fin[3, pl.ds(s, 1), :]
            t_r, t_i = a_r * t_r - a_i * t_i, a_r * t_i + a_i * t_r
            u_r, u_i = a_r * u_r - a_i * u_i + b_r, a_r * u_i + a_i * u_r + b_i
        for c, value in enumerate((t_r, t_i, u_r, u_i)):
            summary[c, pl.ds(k, 1), :] = value
        return carry

    lax.fori_loop(0, tiles, tile, 0)

    def copy(d):
        return pltpu.make_async_remote_copy(
            src_ref=summary, dst_ref=slots.at[d - 1],
            send_sem=send_sem.at[d - 1], recv_sem=recv_sem.at[d - 1],
            device_id={"sp": lax.rem(me + d, n_sp)},
            device_id_type=pl.DeviceIdType.MESH,
        )

    before[...] = jnp.zeros_like(before)
    if n_sp > 1:
        pl.semaphore_wait(barrier, n_sp - 1)
        for d in range(1, n_sp):
            @pl.when(me + d < n_sp)
            def _():
                copy(d).start()

    for start in range(0, resp.shape[1], LANES):
        at = pl.ds(start, LANES)
        resp[:, at] = skip_ref[:, at] * x_ref[:, at].astype(jnp.float32)

    for d in range(n_sp - 1, 0, -1):
        @pl.when(me >= d)
        def _():
            copy(d).wait_recv()
            a_r, a_i = slots[d - 1, 0], slots[d - 1, 1]
            h_r, h_i = before[0], before[1]
            before[0] = a_r * h_r - a_i * h_i + slots[d - 1, 2]
            before[1] = a_r * h_i + a_i * h_r + slots[d - 1, 3]

    def finish(k, carry):
        block = pl.multiple_of((k // tiles_per_block) * LANES, LANES)
        h_r, h_i = before[0, pl.ds(k, 1), :], before[1, pl.ds(k, 1), :]
        t_r, t_i = excl[0, k], excl[1, k]
        o_r = t_r * h_r - t_i * h_i + excl[2, k]
        o_i = t_r * h_i + t_i * h_r + excl[3, k]
        for s in range(SEGMENTS):
            at = pl.ds(s * span, span)
            b_r, b_i = o_r[s : s + 1, :], o_i[s : s + 1, :]
            a_r, a_i = pr[k, at, :], pi[k, at, :]
            packed[at, :LANES] = (sr[k, at, :] + a_r * b_r - a_i * b_i).astype(jnp.bfloat16)
            packed[at, LANES:] = (si[k, at, :] + a_r * b_i + a_i * b_r).astype(jnp.bfloat16)
        resp[:, pl.ds(block, LANES)] += jnp.dot(
            packed[...], w_out_ref[k], preferred_element_type=jnp.float32
        )
        return carry

    lax.fori_loop(0, tiles, finish, 0)
    for start in range(0, resp.shape[1], LANES):
        at = pl.ds(start, LANES)
        out_ref[:, at] = jax.nn.gelu(resp[:, at]).astype(out_ref.dtype)
    for d in range(1, n_sp):
        @pl.when(me + d < n_sp)
        def _():
            copy(d).wait_send()


def state_space(n_sp, x, step_log, forget_log, rate, freq, in_map, out_map, skip):
    rows, local_width = x.shape
    _, groups, entries, channels = in_map.shape
    per_tile = LANES // entries
    tiles = groups // per_tile
    per_block = LANES // channels
    tiles_per_block = per_block // per_tile
    a_real = -rate.reshape(tiles, LANES)
    omega = freq.reshape(tiles, LANES)
    divisor = a_real * a_real + omega * omega
    rates = jnp.stack([a_real, omega, a_real / divisor, omega / divisor])
    slot = jnp.arange(per_block)[None, :, None]
    own = per_tile * (jnp.arange(tiles) % tiles_per_block)
    mask = slot == own[:, None, None] + jnp.arange(per_tile)[None, None, :]
    w_in = in_map.astype(jnp.bfloat16).reshape(2, tiles, per_tile, entries, channels).transpose(1, 4, 0, 2, 3)
    w_in = jnp.where(mask[:, :, None, None, :, None], w_in[:, None], 0).reshape(tiles, LANES, 2 * LANES)
    sign = jnp.array([1.0, -1.0], jnp.float32)[:, None, None, None]
    w_out = (out_map * sign).astype(jnp.bfloat16).reshape(2, tiles, per_tile, channels, entries)
    w_out = w_out.transpose(1, 0, 2, 4, 3)[:, :, :, :, None, :]
    w_out = jnp.where(mask.transpose(0, 2, 1)[:, None, :, None, :, None], w_out, 0)
    w_out = w_out.reshape(tiles, 2 * LANES, LANES)
    vmem = pl.BlockSpec(memory_space=pltpu.VMEM)
    f32 = jnp.float32
    peers = max(n_sp - 1, 1)
    big = pltpu.VMEM((tiles, rows, LANES), f32)
    return pl.pallas_call(
        functools.partial(ssm_kernel, n_sp, groups, per_tile, tiles_per_block),
        out_shape=jax.ShapeDtypeStruct((rows, local_width), jnp.bfloat16),
        in_specs=[vmem] * 7,
        out_specs=vmem,
        scratch_shapes=[
            pltpu.VMEM(step_log.shape, f32), pltpu.VMEM(step_log.shape, f32),
            big, big, big, big,
            pltpu.VMEM((4, SEGMENTS, LANES), f32),
            pltpu.VMEM((4, tiles, SEGMENTS, LANES), f32),
            pltpu.VMEM((4, tiles, LANES), f32),
            pltpu.VMEM((peers, 4, tiles, LANES), f32),
            pltpu.VMEM((2, tiles, LANES), f32),
            pltpu.VMEM((rows, 2 * LANES), jnp.bfloat16),
            pltpu.VMEM((rows, local_width), f32),
            pltpu.SemaphoreType.DMA((peers,)),
            pltpu.SemaphoreType.DMA((peers,)),
        ],
        compiler_params=pltpu.CompilerParams(
            collective_id=0, has_side_effects=True, vmem_limit_bytes=40 * 2**20,
        ),
        cost_estimate=pl.CostEstimate(
            flops=60_000_000_000, bytes_accessed=4_000_000, transcendentals=0
        ),
    )(x, step_log, forget_log, rates, w_in, w_out, skip)


def ring_tables(n):
    if n % 2:
        return list(range(n))
    return list(range(0, n, 2)) + list(range(n - 1, 0, -2))


def ring_owner(n, position):
    if n % 2:
        return position
    return jnp.where(position < n // 2, 2 * position, 2 * (n - 1 - position) + 1)


def ring_position(n, index):
    if n % 2:
        return index
    return jnp.where(index % 2 == 0, index // 2, n - 1 - index // 2)


def ring_steps(halves, n, block, direction):
    order = ring_tables(n)
    route = [
        (side * n + order[i], side * n + order[(i + direction) % n])
        for side in range(halves) for i in range(n)
    ]
    place = ring_position(n, lax.rem(lax.axis_index("sp"), n))
    for step in range(n):
        owner = ring_owner(n, lax.rem(place - direction * step + n * n, n))
        yield block, owner
        if step < n - 1:
            block = lax.ppermute(block, "sp", route)


def scatter_sum(partial, tp_count):
    rows, width = partial.shape
    pieces = lax.all_to_all(
        partial.reshape(tp_count, rows // tp_count, width), "tp", split_axis=0, concat_axis=0, tiled=True
    )
    return jnp.sum(pieces.astype(jnp.float32), axis=0)


def local(
    mixer_input, step_log, forget_log, decay_rate, frequency, input_map, output_map,
    skip_gain, value_weight, gate_weight, residual, norm_gain, ffn_gate, ffn_up,
    conv_taps, ffn_down,
):
    tp_index = lax.axis_index("tp")
    n_sp = lax.axis_size("sp")
    tp_count = lax.axis_size("tp")
    positions, local_width = mixer_input.shape
    groups = input_map.shape[1]
    model = ffn_gate.shape[0] * n_sp
    hidden_width = ffn_gate.shape[1]
    depth = ffn_gate.shape[0]
    wide = ffn_down.shape[1]
    around = n_sp // 2
    side = lax.axis_index("sp") // around
    place = lax.rem(lax.axis_index("sp"), around)
    swap = [(i, (i + around) % n_sp) for i in range(n_sp)]
    half = hidden_width // 2
    first = side == 0

    def halves(left, right):
        return jnp.where(first, left, right), jnp.where(first, right, left)

    gate_own, gate_give = halves(ffn_gate[:, :half], ffn_gate[:, half:])
    up_own, up_give = halves(ffn_up[:, :half], ffn_up[:, half:])
    down_own, down_give = halves(ffn_down[:half], ffn_down[half:])
    gate_got = lax.ppermute(gate_give, "sp", swap)
    up_got = lax.ppermute(up_give, "sp", swap)
    down_got = lax.ppermute(down_give, "sp", swap)

    gate_full = jnp.zeros((model, half), ffn_gate.dtype)
    up_full = jnp.zeros((model, half), ffn_up.dtype)
    down_full = jnp.zeros((half, model), ffn_down.dtype)
    own_base, got_base = side * around, (1 - side) * around
    for base, gate_block, up_block in ((own_base, gate_own, up_own), (got_base, gate_got, up_got)):
        for block, owner in ring_steps(2, around, gate_block, 1):
            gate_full = lax.dynamic_update_slice(gate_full, block, ((base + owner) * depth, 0))
        for block, owner in ring_steps(2, around, up_block, -1):
            up_full = lax.dynamic_update_slice(up_full, block, ((base + owner) * depth, 0))
    for base, down_block, way in ((own_base, down_own, 1), (got_base, down_got, -1)):
        for block, owner in ring_steps(2, around, down_block, way):
            down_full = lax.dynamic_update_slice(down_full, block, (0, (base + owner) * wide))

    activated = state_space(
        n_sp, mixer_input, step_log, forget_log,
        lax.dynamic_slice_in_dim(decay_rate, tp_index * groups, groups, 0),
        lax.dynamic_slice_in_dim(frequency, tp_index * groups, groups, 0),
        input_map, output_map,
        lax.dynamic_slice_in_dim(skip_gain, tp_index * local_width, local_width, 0)[None],
    )
    own_rows = positions // tp_count
    row_block = lax.all_to_all(
        activated.reshape(tp_count, own_rows, local_width),
        "tp", split_axis=0, concat_axis=2, tiled=True,
    )[0]
    value = jnp.dot(row_block, value_weight, preferred_element_type=jnp.float32)
    gate = jnp.dot(row_block, gate_weight, preferred_element_type=jnp.float32)
    mixed = value * jax.nn.sigmoid(gate)
    stream = (residual.astype(jnp.float32) + mixed).astype(jnp.bfloat16)
    stream_wide = stream.astype(jnp.float32)
    scale = lax.rsqrt(jnp.mean(stream_wide * stream_wide, axis=1, keepdims=True) + 1e-06)
    normed = (stream_wide * scale * norm_gain.astype(jnp.float32)).astype(jnp.bfloat16)
    other = lax.ppermute(normed, "sp", swap)
    rows_mine = lax.all_gather(normed, "tp", axis=0, tiled=True)
    rows_other = lax.all_gather(other, "tp", axis=0, tiled=True)

    history = conv_taps.shape[0] - 1
    taps = lax.dynamic_slice_in_dim(conv_taps, tp_index * hidden_width + side * half, half, 1)
    gate_mine = jnp.dot(rows_mine, gate_full, preferred_element_type=jnp.float32)
    gate_other = jnp.dot(rows_other, gate_full, preferred_element_type=jnp.float32)
    tail_mine, tail_other = gate_mine[positions - history :], gate_other[positions - history :]
    tails = jnp.stack(halves(tail_mine, tail_other))
    onward = [
        (s * around + i, s * around + (i + 1) % around) for s in range(2) for i in range(around)
    ]
    came = lax.ppermute(tails, "sp", onward)
    opening = place == 0
    early = jnp.where(opening, 0.0, came[0])
    late = jnp.where(opening, came[0], came[1])
    before_mine, before_other = halves(early, late)

    def hidden_rows(rows, gate_pre, before):
        up_pre = jnp.dot(rows, up_full, preferred_element_type=jnp.float32)
        extended = jnp.concatenate([before, gate_pre], axis=0)
        conv_gate = taps[0] * extended[0:positions]
        for offset in range(1, history + 1):
            conv_gate = conv_gate + taps[offset] * extended[offset : offset + positions]
        return (jax.nn.silu(conv_gate) * up_pre).astype(jnp.bfloat16)

    hidden_other = hidden_rows(rows_other, gate_other, before_other)
    hidden_mine = hidden_rows(rows_mine, gate_mine, before_mine)
    part_other = jnp.dot(hidden_other, down_full, preferred_element_type=jnp.float32).astype(jnp.bfloat16)
    sum_other = scatter_sum(part_other, tp_count).astype(jnp.bfloat16)
    sum_back = lax.ppermute(sum_other, "sp", swap)
    part_mine = jnp.dot(hidden_mine, down_full, preferred_element_type=jnp.float32).astype(jnp.bfloat16)
    sum_mine = scatter_sum(part_mine, tp_count)
    return (stream_wide + sum_mine + sum_back.astype(jnp.float32)).astype(jnp.bfloat16)


def solution(mesh):
    in_specs = (
        P("sp", "tp"), P("sp", None), P("sp", None), P(), P(),
        P(None, "tp", None, None), P(None, "tp", None, None),
        P(), P(), P(), P(("sp", "tp"), None), P(),
        P("sp", "tp"), P("sp", "tp"), P(), P("tp", "sp"),
    )
    out_specs = P(("sp", "tp"), None)
    return jax.shard_map(local, mesh=mesh, in_specs=in_specs, out_specs=out_specs, check_vma=False)
```
